32 devices in a mesh: ep: 16 (over z, y, x), tp: 2 (over core).
Axes of the slice: x: 2, y: 2, z: 4, core: 2. Of those that a mesh axis runs over, the one named last changes fastest.
Arguments:
- tokens: bfloat16 [256, 1024], P('ep'), may hold values from -6 to 6
- mixer_gain: float32 [1024], replicated, may hold values from 0.1 to 1.9
- query_weight: bfloat16 [1024, 1024], P(None, 'tp'), may hold values from -0.1875 to 0.1875
- key_weight: bfloat16 [1024, 256], P(None, 'tp'), may hold values from -0.1875 to 0.1875
- value_weight: bfloat16 [1024, 256], P(None, 'tp'), may hold values from -0.1875 to 0.1875
- head_lambda: float32 [8], P('tp'), may hold values from 0.3 to 0.8
- head_gain: float32 [128], replicated, may hold values from 0.1 to 1.9
- out_weight: bfloat16 [1024, 1024], P('tp'), may hold values from -0.1875 to 0.1875
- cache_keys: bfloat16 [256, 1024, 256], P('ep', None, 'tp'), may hold values from -700 to 700
- cache_values: bfloat16 [256, 1024, 256], P('ep', None, 'tp'), may hold values from -6 to 6
- seq_lengths: int32 [256], P('ep'), may hold values from 2 to 1024, as said below
- channel_gain: float32 [1024], replicated, may hold values from 0.1 to 1.9
- expert_ids: int32 [256, 6], P('ep'), may hold values from 0 to 15, all different within a row; in each aligned block of 16 rows (0 to 15, 16 to 31, ...) at most 12 rows name the same one
- expert_shares: bfloat16 [256, 6], P('ep'), may hold values from 0.19921875 to 1
- expert_gate: bfloat16 [16, 1024, 256], P('ep', None, 'tp'), may hold values from -0.1875 to 0.1875
- expert_up: bfloat16 [16, 1024, 256], P('ep', None, 'tp'), may hold values from -0.1875 to 0.1875
- expert_down: bfloat16 [16, 256, 1024], P('ep', 'tp'), may hold values from -0.375 to 0.375
- dense_gate: bfloat16 [1024, 4096], P('tp', 'ep'), may hold values from -0.1875 to 0.1875
- dense_up: bfloat16 [1024, 4096], P('tp', 'ep'), may hold values from -0.1875 to 0.1875
- dense_down: bfloat16 [4096, 1024], P('ep', 'tp'), may hold values from -0.1875 to 0.1875
- branch_gate: float32 [1024], replicated, may hold values from -0.1875 to 0.1875
Outputs:
- layer_out: bfloat16 [256, 1024], P('ep', 'tp')
The draws below stay inside these ranges and needn't reach their ends.
Inputs may be any that keep to these rules, and one draw needn't show every extreme that they name: `expert_ids`: each row names 6 different experts; among the 16 rows of one index of ep no expert is named by more than 12 rows. `seq_lengths`: some sequence has all 1024 positions live.
All inputs are finite; a program needn't handle non-finite values.
Results may differ from the reference program's by a relative error of at most 0.017.
The reference program's roundings to bfloat16 on the way count: a program that leaves them out, or rounds other values in their place, can miss the bound.
Values may be sent and summed in bfloat16 or wider, within the bound.
A program may use at most 64 MiB of HBM per device.

```python
import math
import jax
import jax.numpy as jnp
import numpy as np
from jax import lax

D = 1024
H = 8
KG = 2
HD = 64
VD = 128
F = 256
DH = 4096
TOP_K = 6
SEQ_DEV = 16
CACHE_LEN = 1024
BATCH = 256
EXPERTS = 16
CAP = 12
N_EP = 16


def draw_cache_keys(key, part):
    base_key = jax.random.fold_in(key, 17)
    first_key = jax.random.fold_in(base_key, 0)
    normal_draw = jnp.clip(jax.random.normal(first_key, (BATCH, CACHE_LEN, KG * 2 * HD), jnp.float32), -6.0, 6.0) * 1.75
    return normal_draw.astype(jnp.bfloat16)


def draw_seq_lengths(key, part):
    base_key = jax.random.fold_in(key, 29)
    first_key, second_key = jax.random.split(base_key)
    base_draw = jax.random.randint(first_key, (BATCH,), 0, CACHE_LEN - 1)
    level_draw = jax.random.randint(second_key, (BATCH // SEQ_DEV,), 1, 5)
    levels = jnp.repeat(level_draw, SEQ_DEV)
    lengths = 2 + base_draw * levels // 4
    lengths = lengths.at[0].set(CACHE_LEN)
    return lengths.astype(jnp.int32)


def shard_levels(rng, dims, shards, smallest, top_value):
    loudness, own = 1.0, jax.random.fold_in(rng, 6)
    for dim, blocks in shards:
        draws = jnp.exp(jax.random.uniform(jax.random.fold_in(own, dim), (blocks,), jnp.float32, smallest / len(shards), top_value / len(shards)))
        loudness = loudness * jnp.repeat(draws, dims[dim] // blocks).reshape([-1 if axis == dim else 1 for axis in range(len(dims))])
    return loudness


def routed_block(stream_key, own, number, rows, count, top, most, slope):
    order = jax.random.permutation(stream_key, count)
    heavy_load, ordinary = portions_of(count, rows * top, most, slope, True), portions_of(count, rows * top, most, slope, False)
    places = jnp.arange(count)

    def named(sizes, offset_by):
        used = int((sizes > 0).sum())
        fixed = max(1, used // 4)
        moved = fixed + (places - fixed + offset_by * (used - fixed)) % max(1, count - fixed)
        return jnp.zeros((count,), jnp.int32).at[order[jnp.where(places < fixed, places, moved)]].set(jnp.asarray(sizes, jnp.int32))

    sizes = jnp.where(number % 4 == 0, named(heavy_load, number // 4), named(ordinary, number - number // 4 - 1))
    mixed = jax.random.permutation(jax.random.fold_in(own, 3), count)
    donor, receiver = mixed[0:count // 2 * 2:2], mixed[1:count // 2 * 2:2]
    room = jnp.minimum(sizes[donor] - 1, most - sizes[receiver]) // 2
    room = jnp.where((donor == order[0]) | (receiver == order[0]) | (sizes[receiver] == 0), 0, jnp.maximum(room, 0))
    moved = jax.random.randint(jax.random.fold_in(own, 4), (count // 2,), 0, 1 << 20) % (room + 1)
    sizes = sizes.at[donor].add(-moved).at[receiver].add(moved)
    members = jnp.searchsorted(jnp.cumsum(sizes), jnp.arange(rows * top), side="right").astype(jnp.int32)
    table = members.reshape(top, rows).T
    table = table[jax.random.permutation(jax.random.fold_in(own, 1), rows)]
    offset_by = jax.random.randint(jax.random.fold_in(own, 2), (rows, 1), 0, top)
    return jnp.take_along_axis(table, (jnp.arange(top)[None, :] + offset_by) % top, axis=1)


def portions_of(amount, total, limit, slope, full):
    weights = [(1 << 20) // math.isqrt(standing ** slope) + 1 for standing in range(1, amount + 1)]
    largest = limit if full else min(limit, max(-(-total // amount), total * weights[0] // sum(weights)))
    least = 1 if total - largest >= amount - 1 else 0
    given, rest = [largest] + [least] * (amount - 1), total - largest - least * (amount - 1)
    while rest > 0:
        candidates = [i for i in range(1, amount) if given[i] < largest] or [i for i in range(1, amount) if given[i] < limit]
        mass, remaining = sum([weights[i] for i in candidates]), rest
        for i in candidates:
            addition = min(limit - given[i], max(1, remaining * weights[i] // mass), rest)
            given[i] = given[i] + addition
            rest = rest - addition
    return np.array(given)


def normal_values(stream_key, dims, spread, reach, shards=(), kind=jnp.bfloat16):
    values = spread * jax.random.normal(stream_key, dims, jnp.float32)
    if shards:
        values = values * shard_levels(stream_key, dims, shards, -0.22, 0.18)
    return jnp.clip(values, -reach, reach).astype(kind)


def setup_inputs(seed: int = 0) -> dict:
    streams_of = jax.random.split(jax.random.key(seed), 22)
    tokens = normal_values(streams_of[0], (BATCH, D), 1.0, 6.0, ((0, 16),))
    mixer_gain = jnp.clip(1.0 + 0.18 * jax.random.normal(streams_of[1], (D,), jnp.float32), 0.1, 1.9)
    query_weight = normal_values(streams_of[2], (D, H * 2 * HD), D ** -0.5, 0.1875, ((1, 2),))
    key_weight = normal_values(streams_of[3], (D, KG * 2 * HD), D ** -0.5, 0.1875, ((1, 2),))
    value_weight = normal_values(streams_of[4], (D, KG * VD), D ** -0.5, 0.1875, ((1, 2),))
    head_lambda = jnp.clip(0.3 + 0.5 * jax.random.uniform(streams_of[5], (H,), jnp.float32) ** shard_levels(streams_of[5], (H,), ((0, 2),), -0.2, 0.2), 0.3, 0.8)
    head_gain = jnp.clip(1.0 + 0.18 * jax.random.normal(streams_of[6], (VD,), jnp.float32), 0.1, 1.9)
    out_weight = normal_values(streams_of[7], (H * VD, D), (H * VD) ** -0.5, 0.1875, ((0, 2),))
    cache_keys = draw_cache_keys(jax.random.fold_in(streams_of[21], 71), 0)
    cache_values = normal_values(streams_of[9], (BATCH, CACHE_LEN, KG * VD), 1.0, 6.0, ((0, 16), (2, 2)))
    seq_lengths = draw_seq_lengths(jax.random.fold_in(streams_of[21], 71), 0)
    channel_gain = jnp.clip(1.0 + 0.18 * jax.random.normal(streams_of[11], (D,), jnp.float32), 0.1, 1.9)
    expert_ids_keys = jax.random.split(jax.random.fold_in(streams_of[12], 1), BATCH // SEQ_DEV)
    expert_ids_turns = jax.random.permutation(jax.random.fold_in(streams_of[12], 3), BATCH // SEQ_DEV)
    expert_ids = jax.vmap(lambda own, number: routed_block(jax.random.fold_in(streams_of[12], 2), own, number, SEQ_DEV, EXPERTS, TOP_K, CAP, 2))(expert_ids_keys, expert_ids_turns).reshape((BATCH, TOP_K))
    expert_shares = jnp.clip(0.19921875 + 0.80078125 * jax.random.uniform(streams_of[13], (BATCH, TOP_K), jnp.float32) ** shard_levels(streams_of[13], (BATCH, TOP_K), ((0, 16),), -0.2, 0.2), 0.19921875, 1.0).astype(jnp.bfloat16)
    expert_gate = normal_values(streams_of[14], (EXPERTS, D, F), D ** -0.5, 0.1875, ((0, 16), (2, 2)))
    expert_up = normal_values(streams_of[15], (EXPERTS, D, F), D ** -0.5, 0.1875, ((0, 16), (2, 2)))
    expert_down = normal_values(streams_of[16], (EXPERTS, F, D), F ** -0.5, 0.375, ((0, 16), (1, 2)))
    dense_gate = normal_values(streams_of[17], (D, DH), D ** -0.5, 0.1875, ((0, 2), (1, 16)))
    dense_up = normal_values(streams_of[18], (D, DH), D ** -0.5, 0.1875, ((0, 2), (1, 16)))
    dense_down = normal_values(streams_of[19], (DH, D), (DH // 4) ** -0.5, 0.1875, ((0, 16), (1, 2)))
    branch_gate = normal_values(streams_of[20], (D,), D ** -0.5, 0.1875, (), jnp.float32)
    return dict(tokens=tokens, mixer_gain=mixer_gain, query_weight=query_weight, key_weight=key_weight, value_weight=value_weight, head_lambda=head_lambda, head_gain=head_gain, out_weight=out_weight, cache_keys=cache_keys, cache_values=cache_values, seq_lengths=seq_lengths, channel_gain=channel_gain, expert_ids=expert_ids, expert_shares=expert_shares, expert_gate=expert_gate, expert_up=expert_up, expert_down=expert_down, dense_gate=dense_gate, dense_up=dense_up, dense_down=dense_down, branch_gate=branch_gate)


NORM_EPS = 1e-06
HEAD_EPS = 1e-05
THETA = 500000.0
LAMBDA_BASE = 0.2

def norm_rows(values, gain_vec, epsilon):
    mean_square = lax.optimization_barrier(jnp.mean(values * values, axis=-1, keepdims=True))
    return values * lax.rsqrt(mean_square + epsilon) * gain_vec

def rotate(values, position):
    half_dim = HD // 2
    frequency = THETA ** (-jnp.arange(half_dim, dtype=jnp.float32) * (2.0 / HD))
    angles = position.astype(jnp.float32)[:, None] * frequency[None, :]
    cos_vals = jnp.cos(angles)[:, None, :]
    sin_vals = jnp.sin(angles)[:, None, :]
    first_half = values[..., :half_dim]
    second = values[..., half_dim:]
    return jnp.concatenate([first_half * cos_vals - second * sin_vals, second * cos_vals + first_half * sin_vals], axis=-1)

def widen(values):
    return values.astype(jnp.float32)

def reference(tokens, mixer_gain, query_weight, key_weight, value_weight, head_lambda, head_gain, out_weight, cache_keys, cache_values, seq_lengths, channel_gain, expert_ids, expert_shares, expert_gate, expert_up, expert_down, dense_gate, dense_up, dense_down, branch_gate):
    resid = widen(tokens)
    normed = norm_rows(resid, mixer_gain, NORM_EPS).astype(jnp.bfloat16)
    query_raw = jnp.dot(normed, query_weight, preferred_element_type=jnp.float32).reshape(BATCH, H * 2, HD)
    key_raw = jnp.dot(normed, key_weight, preferred_element_type=jnp.float32).reshape(BATCH, KG * 2, HD)
    value_new = jnp.dot(normed, value_weight, preferred_element_type=jnp.float32).astype(jnp.bfloat16)
    value_new = value_new.reshape(N_EP, SEQ_DEV, KG, VD)
    query = rotate(query_raw, seq_lengths).astype(jnp.bfloat16).reshape(N_EP, SEQ_DEV, KG, H // KG, 2, HD)
    key_new = rotate(key_raw, seq_lengths).astype(jnp.bfloat16).reshape(N_EP, SEQ_DEV, KG, 2, HD)
    lambdas = head_lambda.reshape(KG, H // KG)
    key_rows = cache_keys.reshape(N_EP, SEQ_DEV, CACHE_LEN, KG, 2, HD)
    value_rows = cache_values.reshape(N_EP, SEQ_DEV, CACHE_LEN, KG, VD)
    length_rows = seq_lengths.reshape(N_EP, SEQ_DEV)
    score_scale = HD ** (-0.5)

    def attend_block(pieces_in):
        query_blk, key_blk, value_blk, cache_key_blk, cache_value_blk, length_blk = pieces_in
        scores = jnp.einsum('sgjcd,slgcd->sgjcl', widen(query_blk), widen(cache_key_blk)) * score_scale
        fresh_score = jnp.einsum('sgjcd,sgcd->sgjc', widen(query_blk), widen(key_blk)) * score_scale
        live = jnp.arange(CACHE_LEN)[None, :] < length_blk[:, None]
        scores = jnp.where(live[:, None, None, None, :], scores, -jnp.inf)
        peak = jnp.maximum(lax.optimization_barrier(jnp.max(scores, axis=-1)), fresh_score)
        expo_scores = jnp.exp(scores - peak[..., None])
        expo_fresh = jnp.exp(fresh_score - peak)
        denom_sum = lax.optimization_barrier(jnp.sum(expo_scores, axis=-1)) + expo_fresh
        probability = expo_scores / denom_sum[..., None]
        prob_fresh = expo_fresh / denom_sum
        weight = (probability[:, :, :, 0] - lambdas[None, :, :, None] * probability[:, :, :, 1]).astype(jnp.bfloat16)
        weight_fresh = (prob_fresh[..., 0] - lambdas[None] * prob_fresh[..., 1]).astype(jnp.bfloat16)
        mixed_heads = jnp.einsum('sgjl,slgv->sgjv', widen(weight), widen(cache_value_blk))
        return mixed_heads + widen(weight_fresh)[..., None] * widen(value_blk)[:, :, None, :]
    head_mix = lax.map(attend_block, (query, key_new, value_new, key_rows, value_rows, length_rows))
    head_mix = head_mix.reshape(BATCH, H, VD)
    head_out = (norm_rows(head_mix, head_gain, HEAD_EPS) * (1.0 - LAMBDA_BASE)).astype(jnp.bfloat16)
    attn_sum = jnp.dot(head_out.reshape(BATCH, H * VD), out_weight, preferred_element_type=jnp.float32)
    resid_mid = (resid + attn_sum).astype(jnp.bfloat16)
    mid_wide = widen(resid_mid)
    ffn_input = norm_rows(mid_wide, channel_gain, NORM_EPS).astype(jnp.bfloat16)
    gate_value = jax.nn.sigmoid(jnp.dot(widen(ffn_input), branch_gate, precision=lax.Precision.HIGHEST))
    dense_gate_part = jnp.dot(ffn_input, dense_gate, preferred_element_type=jnp.float32)
    dense_up_part = jnp.dot(ffn_input, dense_up, preferred_element_type=jnp.float32)
    dense_hidden = (jax.nn.silu(dense_gate_part) * dense_up_part).astype(jnp.bfloat16)
    dense_sum = jnp.dot(dense_hidden, dense_down, preferred_element_type=jnp.float32)
    padded_rows = jnp.concatenate([ffn_input, jnp.zeros((1, D), ffn_input.dtype)], axis=0)
    share_wide = widen(expert_shares)

    def expert_step(running, pieces_in):
        gate_mat, up_mat, down_mat, expert_index = pieces_in
        named_mask = expert_ids == expert_index
        picked = jnp.any(named_mask, axis=1)
        row_share = lax.optimization_barrier(jnp.sum(jnp.where(named_mask, share_wide, jnp.zeros_like(share_wide)), axis=1))
        row_share = jnp.concatenate([row_share, jnp.zeros((1,), row_share.dtype)])
        row_index = jnp.nonzero(picked, size=N_EP * CAP, fill_value=BATCH)[0].astype(jnp.int32)
        chosen_rows = padded_rows[row_index]
        gate_part = jnp.dot(chosen_rows, gate_mat, preferred_element_type=jnp.float32)
        up_part = jnp.dot(chosen_rows, up_mat, preferred_element_type=jnp.float32)
        expert_hidden = (jax.nn.silu(gate_part) * up_part).astype(jnp.bfloat16)
        expert_row = jnp.dot(expert_hidden, down_mat, preferred_element_type=jnp.float32).astype(jnp.bfloat16)
        running = running.at[row_index].add(row_share[row_index][:, None] * widen(expert_row))
        return (running, None)
    running = jnp.zeros((BATCH + 1, D), jnp.float32)
    running, _ = lax.scan(expert_step, running, (expert_gate, expert_up, expert_down, jnp.arange(EXPERTS, dtype=jnp.int32)))
    routed = running[:BATCH]
    return (mid_wide + routed + gate_value[:, None] * dense_sum).astype(jnp.bfloat16)
```

```python
import functools

import jax
import jax.numpy as jnp
from jax import lax
from jax.experimental import pallas as pl
from jax.experimental.pallas import tpu as pltpu
from jax.sharding import PartitionSpec as P

HD = 64
NORM_EPS = 1e-06
HEAD_EPS = 1e-05
THETA = 500000.0
LAMBDA_BASE = 0.2
MESH = pl.DeviceIdType.MESH
F32 = jnp.float32
BF16 = jnp.bfloat16


def norm_rows(values, gain_vec, epsilon):
    mean_square = jnp.mean(values * values, axis=-1, keepdims=True)
    return values * lax.rsqrt(mean_square + epsilon) * gain_vec


def mm(a, b):
    return jnp.dot(a, b, preferred_element_type=F32)


def attend_kernel(
    heads, block, len_ref, lam_ref, tok_ref, gain_ref, wq_ref, wk_ref, wv_ref,
    cos_ref, sin_ref, hgain_ref, wo_ref, k_ref, v_ref, out_ref, q8, knew, vnew, mixed,
):
    step = pl.program_id(0)
    wide = 2 * HD
    seqs = tok_ref.shape[0]

    @pl.when(step == 0)
    def _():
        resid = tok_ref[...].astype(F32)
        normed = norm_rows(resid, gain_ref[...], NORM_EPS).astype(BF16)
        lane = lax.broadcasted_iota(jnp.int32, (seqs, wide), 1)
        first = (lane % HD) < HD // 2

        def rotate(x):
            swapped = jnp.where(
                first, pltpu.roll(x, wide - HD // 2, 1), pltpu.roll(x, HD // 2, 1)
            )
            return (x * cos_ref[...] + swapped * sin_ref[...]).astype(BF16).astype(F32)

        raw = mm(normed, wq_ref[...])
        for j in range(heads):
            rotated = rotate(raw[:, j * wide:(j + 1) * wide])
            q8[:, j, :] = jnp.where(lane < HD, rotated, 0.0)
            q8[:, heads + j, :] = jnp.where(lane < HD, 0.0, rotated)
        knew[...] = rotate(mm(normed, wk_ref[...]))
        vnew[...] = mm(normed, wv_ref[...]).astype(BF16).astype(F32)

    scale = HD ** (-0.5)
    span = k_ref.shape[1]
    position = lax.broadcasted_iota(jnp.int32, (2 * heads, span), 1)
    lam_rows = lax.broadcasted_iota(jnp.int32, (heads, 1), 0)
    lam = jnp.zeros((heads, 1), F32)
    for j in range(heads):
        lam = jnp.where(lam_rows == j, lam_ref[j], lam)
    for b in range(block):
        s = step * block + b
        query = q8[s]
        scores = lax.dot_general(
            query.astype(BF16), k_ref[b], (((1,), (1,)), ((), ())), preferred_element_type=F32
        ) * scale
        fresh = jnp.sum(query * knew[pl.ds(s, 1), :], axis=1, keepdims=True) * scale
        scores = jnp.where(position < len_ref[s], scores, -jnp.inf)
        peak = jnp.maximum(jnp.max(scores, axis=1, keepdims=True), fresh)
        expo = jnp.exp(scores - peak)
        expo_fresh = jnp.exp(fresh - peak)
        denom = jnp.sum(expo, axis=1, keepdims=True) + expo_fresh
        prob = expo / denom
        prob_fresh = expo_fresh / denom
        weight = (prob[:heads] - lam * prob[heads:]).astype(BF16)
        weight_fresh = (prob_fresh[:heads] - lam * prob_fresh[heads:]).astype(BF16).astype(F32)
        mix = mm(weight, v_ref[b]) + weight_fresh * vnew[pl.ds(s, 1), :]
        done = norm_rows(mix, hgain_ref[...], HEAD_EPS) * (1.0 - LAMBDA_BASE)
        for j in range(heads):
            mixed[j, pl.ds(s, 1), :] = done[j:j + 1]

    @pl.when(step == pl.num_programs(0) - 1)
    def _():
        rows = jnp.concatenate([mixed[j].astype(BF16) for j in range(heads)], axis=1)
        out_ref[...] = mm(rows, wo_ref[...])


def attend(tokens, mixer_gain, wq, wk, wv, head_lambda, head_gain, wo, keys, values, lengths):
    seqs, width = tokens.shape
    span = keys.shape[1]
    heads = head_lambda.shape[0]
    wide = 2 * HD
    block = 4 if seqs % 4 == 0 else 1
    half = HD // 2
    frequency = THETA ** (-jnp.arange(half, dtype=F32) * (2.0 / HD))
    angles = lengths.astype(F32)[:, None] * frequency[None, :]
    cos_vals = jnp.cos(angles)
    sin_vals = jnp.sin(angles)
    cos_wide = jnp.concatenate([cos_vals] * 4, axis=1)
    sin_wide = jnp.concatenate([-sin_vals, sin_vals] * 2, axis=1)

    def whole(x):
        return pl.BlockSpec(x.shape, lambda i: (0,) * x.ndim)

    smem = pl.BlockSpec(memory_space=pltpu.SMEM)
    gain2 = mixer_gain.reshape(1, -1)
    hgain2 = head_gain.reshape(1, -1)
    stream = pl.BlockSpec((block, span, wide), lambda i: (i, 0, 0))
    return pl.pallas_call(
        functools.partial(attend_kernel, heads, block),
        grid=(seqs // block,),
        out_shape=jax.ShapeDtypeStruct((seqs, width), F32),
        in_specs=[smem, smem, whole(tokens), whole(gain2), whole(wq), whole(wk), whole(wv),
                  whole(cos_wide), whole(sin_wide), whole(hgain2), whole(wo), stream, stream],
        out_specs=pl.BlockSpec((seqs, width), lambda i: (0, 0)),
        scratch_shapes=[
            pltpu.VMEM((seqs, 2 * heads, wide), F32),
            pltpu.VMEM((seqs, wide), F32),
            pltpu.VMEM((seqs, wide), F32),
            pltpu.VMEM((heads, seqs, wide), F32),
        ],
        compiler_params=pltpu.CompilerParams(dimension_semantics=("arbitrary",)),
        name="attend",
    )(lengths, head_lambda, tokens, gain2, wq, wk, wv, cos_wide, sin_wide, hgain2, wo, keys, values)


def ffn_kernel(
    n, parts, ids_ref, shares_ref, tok_ref, attn_ref, cgain_ref, bgate_ref,
    eg, eu, ed, dg, du, dd, out_ref,
    g, table, attn_in, egb, eub, edb, dgb, dub, ddb, pbuf, arrived,
    xsem, lsem, wsend, wrecv, shsend, shrecv, agsend, agrecv, fwsend, fwrecv, rssend, rsrecv,
):
    me = lax.axis_index("ep")
    t = lax.axis_index("tp")
    mate = 1 - t
    seqs, width = tok_ref.shape
    half = width // 2
    size = n // parts
    mine = me // size
    slot = me % size

    barrier = pltpu.get_barrier_semaphore()
    pl.semaphore_signal(barrier, inc=1, device_id=(me, mate), device_id_type=MESH)

    def greet(d, carry):
        pl.semaphore_signal(
            barrier, inc=1, device_id=((me + d) % n, t), device_id_type=MESH
        )
        return carry

    lax.fori_loop(1, n, greet, 0)

    fh = eg.shape[2]
    uh = dg.shape[0]
    own_cols = pl.ds(pl.multiple_of(t * fh, fh), fh)
    own_rows = pl.ds(pl.multiple_of(t * fh, fh), fh)
    own_feats = pl.ds(pl.multiple_of(t * uh, uh), uh)
    my_half = pl.ds(pl.multiple_of(t * half, half), half)
    mate_half = pl.ds(pl.multiple_of(mate * half, half), half)
    local = [
        (eg.at[0], egb.at[:, own_cols]),
        (eu.at[0], eub.at[:, own_cols]),
        (dg, dgb.at[own_feats, :]),
        (du, dub.at[own_feats, :]),
        (ed.at[0, :, my_half], edb.at[own_rows, :]),
        (dd, ddb),
    ]
    local = [pltpu.make_async_copy(a, b, lsem.at[i]) for i, (a, b) in enumerate(local)]
    for copy in local:
        copy.start()
    remote = [
        (eg.at[0], egb.at[:, own_cols]),
        (eu.at[0], eub.at[:, own_cols]),
        (dg, dgb.at[own_feats, :]),
        (du, dub.at[own_feats, :]),
        (ed.at[0, :, mate_half], edb.at[own_rows, :]),
    ]
    remote = [
        pltpu.make_async_remote_copy(a, b, wsend.at[i], wrecv.at[i],
                                     device_id=(me, mate), device_id_type=MESH)
        for i, (a, b) in enumerate(remote)
    ]

    lanes = table.shape[2]
    lane = lax.broadcasted_iota(jnp.int32, (seqs, lanes), 1)
    shares = jnp.zeros((seqs, lanes), F32)
    for k in range(ids_ref.shape[1]):
        shares += jnp.where(
            lane == ids_ref[:, k:k + 1], shares_ref[:, k:k + 1].astype(F32), 0.0
        )
    table[me] = shares.astype(BF16)

    pl.semaphore_wait(barrier, n)

    swap = pltpu.make_async_remote_copy(
        attn_ref, attn_in, xsem.at[0], xsem.at[1], device_id=(me, mate), device_id_type=MESH
    )
    swap.start()
    for copy in remote:
        copy.start()

    def to_peer(buffer, where, sends, recvs, peer):
        return pltpu.make_async_remote_copy(
            buffer.at[where], buffer.at[where], sends.at[peer], recvs.at[me],
            device_id=(peer, t), device_id_type=MESH,
        )

    def landed(buffer, where, sends, recvs, source):
        return pltpu.make_async_remote_copy(
            buffer.at[where], buffer.at[where], sends.at[source], recvs.at[source],
            device_id=(source, t), device_id_type=MESH,
        )

    def each(offset, visit):
        chunk = (mine + offset + parts) % parts

        def body(q, carry):
            peer = chunk * size + (slot + q) % size

            @pl.when(peer != me)
            def _():
                visit(peer)

            return carry

        lax.fori_loop(0, size, body, 0)
        return chunk

    for k in range(parts):
        each(-k, lambda peer: to_peer(table, me, shsend, shrecv, peer).start())

    swap.wait()
    attn_sum = attn_ref[...] + attn_in[...]
    mid = (tok_ref[...].astype(F32) + attn_sum).astype(BF16)
    wide_mid = mid.astype(F32)
    ffn_input = norm_rows(wide_mid, cgain_ref[...], NORM_EPS).astype(BF16)
    g[0, me] = ffn_input[:, :half]
    g[1, me] = ffn_input[:, half:]

    for k in range(parts):
        each(-k, lambda peer: to_peer(g, (t, me), agsend, agrecv, peer).start())

    def forward(source):
        return pltpu.make_async_remote_copy(
            g.at[t, source], g.at[t, source], fwsend.at[source], fwrecv.at[source],
            device_id=(me, mate), device_id_type=MESH,
        )

    def forwarded(source):
        return pltpu.make_async_remote_copy(
            g.at[mate, source], g.at[mate, source], fwsend.at[source], fwrecv.at[source],
            device_id=(me, mate), device_id_type=MESH,
        )

    def relay(source):
        landed(g, (t, source), agsend, agrecv, source).wait_recv()
        forward(source).start()

    def settle(source):
        forwarded(source).wait_recv()
        landed(table, source, shsend, shrecv, source).wait_recv()

    def send_back(peer):
        pltpu.make_async_remote_copy(
            pbuf.at[peer], arrived.at[me], rssend.at[peer], rsrecv.at[me],
            device_id=(peer, t), device_id_type=MESH,
        ).start()

    rows = size * seqs
    pick = lax.broadcasted_iota(jnp.int32, (rows, lanes), 1) == me
    for k in range(parts):
        chunk = each(k, relay)
        if k == 0:
            for copy in local:
                copy.wait()
            for copy in remote:
                copy.wait()
        each(k, settle)
        span = pl.ds(chunk * size, size)
        low = g[0, span].reshape(rows, half)
        high = g[1, span].reshape(rows, half)

        def product(weight):
            return mm(low, weight[:half]) + mm(high, weight[half:])

        gate_logit = jnp.sum(low.astype(F32) * bgate_ref[:, :half], axis=1, keepdims=True) + jnp.sum(
            high.astype(F32) * bgate_ref[:, half:], axis=1, keepdims=True
        )
        gate_value = jax.nn.sigmoid(gate_logit)
        share = jnp.sum(
            jnp.where(pick, table[span].reshape(rows, lanes).astype(F32), 0.0),
            axis=1, keepdims=True,
        )
        expert_hidden = (jax.nn.silu(product(egb)) * product(eub)).astype(BF16)
        expert_row = mm(expert_hidden, edb[...]).astype(BF16).astype(F32)
        dense_hidden = (jax.nn.silu(product(dgb)) * product(dub)).astype(BF16)
        dense_sum = mm(dense_hidden, ddb[...])
        total = (share * expert_row + gate_value * dense_sum).astype(BF16)
        pbuf[span] = total.reshape(size, seqs, half)
        each(k, send_back)

    arrived[me] = pbuf[me]
    for k in range(parts):
        each(-k, lambda peer: landed(arrived, peer, rssend, rsrecv, peer).wait_recv())

    result = lax.fori_loop(
        0, n, lambda i, acc: acc + arrived[i].astype(F32), jnp.zeros((seqs, half), F32)
    )
    mid_half = jnp.where(t == 0, wide_mid[:, :half], wide_mid[:, half:])
    out_ref[...] = (mid_half + result).astype(BF16)

    def drain(peer):
        to_peer(table, me, shsend, shrecv, peer).wait_send()
        to_peer(g, (t, me), agsend, agrecv, peer).wait_send()
        forward(peer).wait_send()
        pltpu.make_async_remote_copy(
            pbuf.at[peer], arrived.at[me], rssend.at[peer], rsrecv.at[me],
            device_id=(peer, t), device_id_type=MESH,
        ).wait_send()

    for k in range(parts):
        each(k, drain)


def ffn(n, ids, shares, tokens, attn, cgain, bgate, eg, eu, ed, dg, du, dd):
    seqs, width = tokens.shape
    half = width // 2
    lanes = -(-n // 128) * 128
    hidden = 2 * eg.shape[2]
    units = dg.shape[1]
    parts = 4 if n % 4 == 0 else 1
    vmem = pl.BlockSpec(memory_space=pltpu.VMEM)
    anyw = pl.BlockSpec(memory_space=pl.ANY)
    dma = pltpu.SemaphoreType.DMA
    return pl.pallas_call(
        functools.partial(ffn_kernel, n, parts),
        out_shape=jax.ShapeDtypeStruct((seqs, half), BF16),
        in_specs=[vmem] * 6 + [anyw] * 6,
        out_specs=vmem,
        scratch_shapes=[
            pltpu.VMEM((2, n, seqs, half), BF16),
            pltpu.VMEM((n, seqs, lanes), BF16),
            pltpu.VMEM((seqs, width), F32),
            pltpu.VMEM((width, hidden), BF16),
            pltpu.VMEM((width, hidden), BF16),
            pltpu.VMEM((hidden, half), BF16),
            pltpu.VMEM((width, units), BF16),
            pltpu.VMEM((width, units), BF16),
            pltpu.VMEM((units, half), BF16),
            pltpu.VMEM((n, seqs, half), BF16),
            pltpu.VMEM((n, seqs, half), BF16),
            dma((2,)), dma((6,)), dma((5,)), dma((5,)),
            dma((n,)), dma((n,)), dma((n,)), dma((n,)),
            dma((n,)), dma((n,)), dma((n,)), dma((n,)),
        ],
        compiler_params=pltpu.CompilerParams(collective_id=0, has_side_effects=True),
        name="ffn",
    )(ids, shares, tokens, attn, cgain.reshape(1, -1), bgate.reshape(1, -1), eg, eu, ed, dg, du, dd)


def shards(
    tokens, mixer_gain, query_weight, key_weight, value_weight, head_lambda, head_gain,
    out_weight, cache_keys, cache_values, seq_lengths, channel_gain, expert_ids,
    expert_shares, expert_gate, expert_up, expert_down, dense_gate, dense_up, dense_down,
    branch_gate,
):
    attn_part = attend(
        tokens, mixer_gain, query_weight, key_weight, value_weight, head_lambda, head_gain,
        out_weight, cache_keys, cache_values, seq_lengths,
    )
    return ffn(
        lax.axis_size("ep"), expert_ids, expert_shares, tokens, attn_part, channel_gain,
        branch_gate, expert_gate, expert_up, expert_down, dense_gate, dense_up, dense_down,
    )


def solution(mesh):
    placed = (
        P("ep", None), P(), P(None, "tp"), P(None, "tp"), P(None, "tp"), P("tp"), P(),
        P("tp", None), P("ep", None, "tp"), P("ep", None, "tp"), P("ep"), P(),
        P("ep", None), P("ep", None), P("ep", None, "tp"), P("ep", None, "tp"),
        P("ep", "tp", None), P("tp", "ep"), P("tp", "ep"), P("ep", "tp"), P(),
    )
    return jax.shard_map(
        shards, mesh=mesh, in_specs=placed, out_specs=P("ep", "tp"), check_vma=False
    )
```

```python
import functools

import jax
import jax.numpy as jnp
import numpy as np
from jax import lax
from jax.experimental import pallas as pl
from jax.experimental.pallas import tpu as pltpu
from jax.sharding import PartitionSpec as P

HD = 64
NORM_EPS = 1e-06
HEAD_EPS = 1e-05
THETA = 500000.0
LAMBDA_BASE = 0.2
TRIG_STEP = 32
MESH = pl.DeviceIdType.MESH
F32 = jnp.float32
BF16 = jnp.bfloat16


def norm_rows(values, gain_vec, epsilon):
    mean_square = jnp.mean(values * values, axis=-1, keepdims=True)
    return values * lax.rsqrt(mean_square + epsilon) * gain_vec


def mm(a, b):
    return jnp.dot(a, b, preferred_element_type=F32)


def layer_kernel(
    n, parts, block, len_ref, lam_ref, ids_ref, shares_ref, tok_ref, mgain_ref, hgain_ref,
    cgain_ref, bgate_ref, trig_ref, wq_hbm, wk_hbm, wv_hbm, wo_hbm, keys, values,
    eg, eu, ed, dg, du, dd, out_ref,
    wq, wk, wv, wo, kbuf, vbuf, trig, q8, knew, vnew, mixed, attn_ref,
    g, table, attn_in, egb, eub, edb, dgb, dub, ddb, pbuf, arrived,
    psem, ksem, vsem,
    xsem, lsem, wsend, wrecv, shsend, shrecv, agsend, agrecv, fwsend, fwrecv, rssend, rsrecv,
):
    me = lax.axis_index("ep")
    t = lax.axis_index("tp")
    mate = 1 - t
    seqs, width = tok_ref.shape
    half = width // 2
    size = n // parts
    mine = me // size
    slot = me % size

    seq_copies = [
        (
            pltpu.make_async_copy(keys.at[pl.ds(b, block)], kbuf.at[pl.ds(b, block)], ksem.at[b // block]),
            pltpu.make_async_copy(values.at[pl.ds(b, block)], vbuf.at[pl.ds(b, block)], vsem.at[b // block]),
        )
        for b in range(0, seqs, block)
    ]
    projections = [
        pltpu.make_async_copy(a, b, psem.at[i])
        for i, (a, b) in enumerate([(wq_hbm, wq), (wk_hbm, wk), (wv_hbm, wv), (wo_hbm, wo)])
    ]
    for copy in projections[:3]:
        copy.start()
    for pair in seq_copies:
        pair[0].start()
        pair[1].start()
    projections[3].start()

    barrier = pltpu.get_barrier_semaphore()
    pl.semaphore_signal(barrier, inc=1, device_id=(me, mate), device_id_type=MESH)

    def greet(d, carry):
        pl.semaphore_signal(
            barrier, inc=1, device_id=((me + d) % n, t), device_id_type=MESH
        )
        return carry

    lax.fori_loop(1, n, greet, 0)

    fh = eg.shape[2]
    uh = dg.shape[0]
    own_cols = pl.ds(pl.multiple_of(t * fh, fh), fh)
    own_rows = pl.ds(pl.multiple_of(t * fh, fh), fh)
    own_feats = pl.ds(pl.multiple_of(t * uh, uh), uh)
    my_half = pl.ds(pl.multiple_of(t * half, half), half)
    mate_half = pl.ds(pl.multiple_of(mate * half, half), half)
    local = [
        (eg.at[0], egb.at[:, own_cols]),
        (eu.at[0], eub.at[:, own_cols]),
        (dg, dgb.at[own_feats, :]),
        (du, dub.at[own_feats, :]),
        (ed.at[0, :, my_half], edb.at[own_rows, :]),
        (dd, ddb),
    ]
    local = [pltpu.make_async_copy(a, b, lsem.at[i]) for i, (a, b) in enumerate(local)]
    for copy in local:
        copy.start()
    remote = [
        (eg.at[0], egb.at[:, own_cols]),
        (eu.at[0], eub.at[:, own_cols]),
        (dg, dgb.at[own_feats, :]),
        (du, dub.at[own_feats, :]),
        (ed.at[0, :, mate_half], edb.at[own_rows, :]),
    ]
    remote = [
        pltpu.make_async_remote_copy(a, b, wsend.at[i], wrecv.at[i],
                                     device_id=(me, mate), device_id_type=MESH)
        for i, (a, b) in enumerate(remote)
    ]

    lanes = table.shape[2]
    named = lax.broadcasted_iota(jnp.int32, (lanes, seqs), 0)
    shares = jnp.zeros((lanes, seqs), F32)
    for k in range(ids_ref.shape[0]):
        shares += jnp.where(
            named == ids_ref[k:k + 1, :], shares_ref[k:k + 1, :].astype(F32), 0.0
        )
    table[me] = shares.T.astype(BF16)

    wide = 2 * HD
    heads = q8.shape[1] // 2
    for s in range(seqs):
        high = len_ref[s] // TRIG_STEP
        low = len_ref[s] % TRIG_STEP
        cos_h, sin_h = trig_ref[0, pl.ds(high, 1), :], trig_ref[1, pl.ds(high, 1), :]
        cos_l, sin_l = trig_ref[2, pl.ds(low, 1), :], trig_ref[3, pl.ds(low, 1), :]
        trig[0, pl.ds(s, 1), :] = cos_h * cos_l - sin_h * sin_l
        trig[1, pl.ds(s, 1), :] = sin_h * cos_l + cos_h * sin_l
    resid = tok_ref[...].astype(F32)
    normed = norm_rows(resid, mgain_ref[...], NORM_EPS).astype(BF16)
    qlane = lax.broadcasted_iota(jnp.int32, (seqs, wide), 1)
    first = (qlane % HD) < HD // 2
    cos_vals = trig[0]
    sin_vals = jnp.where(first, -trig[1], trig[1])

    def rotate(x):
        swapped = jnp.where(first, pltpu.roll(x, wide - HD // 2, 1), pltpu.roll(x, HD // 2, 1))
        return (x * cos_vals + swapped * sin_vals).astype(BF16).astype(F32)

    for copy in projections[:3]:
        copy.wait()
    raw = mm(normed, wq[...])
    for j in range(heads):
        rotated = rotate(raw[:, j * wide:(j + 1) * wide]) * HD ** (-0.5)
        q8[:, j, :] = jnp.where(qlane < HD, rotated, 0.0)
        q8[:, heads + j, :] = jnp.where(qlane < HD, 0.0, rotated)
    knew[...] = rotate(mm(normed, wk[...]))
    vnew[...] = mm(normed, wv[...]).astype(BF16).astype(F32)

    pl.semaphore_wait(barrier, n)
    for copy in remote:
        copy.start()

    def to_peer(buffer, where, sends, recvs, peer):
        return pltpu.make_async_remote_copy(
            buffer.at[where], buffer.at[where], sends.at[peer], recvs.at[me],
            device_id=(peer, t), device_id_type=MESH,
        )

    def landed(buffer, where, sends, recvs, source):
        return pltpu.make_async_remote_copy(
            buffer.at[where], buffer.at[where], sends.at[source], recvs.at[source],
            device_id=(source, t), device_id_type=MESH,
        )

    def each(offset, visit):
        chunk = (mine + offset + parts) % parts

        def body(q, carry):
            peer = chunk * size + (slot + q) % size

            @pl.when(peer != me)
            def _():
                visit(peer)

            return carry

        lax.fori_loop(0, size, body, 0)
        return chunk

    for k in range(parts):
        each(-k, lambda peer: to_peer(table, me, shsend, shrecv, peer).start())

    cached = kbuf.shape[1]
    tall = 2 * heads
    position = lax.broadcasted_iota(jnp.int32, (block, tall, cached), 2)
    which = lax.broadcasted_iota(jnp.int32, (block, tall, 1), 0)
    lam_rows = lax.broadcasted_iota(jnp.int32, (1, heads, 1), 1)
    lam = jnp.zeros((1, heads, 1), F32)
    for j in range(heads):
        lam = jnp.where(lam_rows == j, lam_ref[j], lam)
    for b0, (key_copy, value_copy) in zip(range(0, seqs, block), seq_copies):
        query = q8[b0:b0 + block]
        fresh = jnp.sum(query * knew[b0:b0 + block][:, None, :], axis=2, keepdims=True)
        live = jnp.zeros((block, tall, 1), jnp.int32)
        for b in range(block):
            live = jnp.where(which == b, len_ref[b0 + b], live)
        key_copy.wait()
        narrow = query.astype(BF16)
        scores = jnp.stack([
            lax.dot_general(narrow[b], kbuf[b0 + b], (((1,), (1,)), ((), ())),
                            preferred_element_type=F32)
            for b in range(block)
        ])
        scores = jnp.where(position < live, scores, -jnp.inf)
        peak = jnp.maximum(jnp.max(scores, axis=2, keepdims=True), fresh)
        expo = jnp.exp(scores - peak)
        expo_fresh = jnp.exp(fresh - peak)
        inverse = 1.0 / (jnp.sum(expo, axis=2, keepdims=True) + expo_fresh)
        prob_fresh = expo_fresh * inverse
        weight = (
            expo[:, :heads] * inverse[:, :heads] - expo[:, heads:] * (lam * inverse[:, heads:])
        ).astype(BF16)
        weight_fresh = (prob_fresh[:, :heads] - lam * prob_fresh[:, heads:]).astype(BF16).astype(F32)
        value_copy.wait()
        mix = jnp.stack([mm(weight[b], vbuf[b0 + b]) for b in range(block)])
        mix = mix + weight_fresh * vnew[b0:b0 + block][:, None, :]
        done = norm_rows(mix, hgain_ref[...], HEAD_EPS) * (1.0 - LAMBDA_BASE)
        for b in range(block):
            for j in range(heads):
                mixed[j, b0 + b:b0 + b + 1, :] = done[b, j:j + 1]
    projections[3].wait()
    rows = jnp.concatenate([mixed[j].astype(BF16) for j in range(heads)], axis=1)
    attn_ref[...] = mm(rows, wo[...])
    swap = pltpu.make_async_remote_copy(
        attn_ref, attn_in, xsem.at[0], xsem.at[1], device_id=(me, mate), device_id_type=MESH
    )
    swap.start()

    swap.wait()
    attn_sum = attn_ref[...] + attn_in[...]
    mid = (tok_ref[...].astype(F32) + attn_sum).astype(BF16)
    wide_mid = mid.astype(F32)
    ffn_input = norm_rows(wide_mid, cgain_ref[...], NORM_EPS).astype(BF16)
    g[0, me] = ffn_input[:, :half]
    g[1, me] = ffn_input[:, half:]

    for k in range(parts):
        each(-k, lambda peer: to_peer(g, (t, me), agsend, agrecv, peer).start())

    def forward(source):
        return pltpu.make_async_remote_copy(
            g.at[t, source], g.at[t, source], fwsend.at[source], fwrecv.at[source],
            device_id=(me, mate), device_id_type=MESH,
        )

    def forwarded(source):
        return pltpu.make_async_remote_copy(
            g.at[mate, source], g.at[mate, source], fwsend.at[source], fwrecv.at[source],
            device_id=(me, mate), device_id_type=MESH,
        )

    def relay(source):
        landed(g, (t, source), agsend, agrecv, source).wait_recv()
        forward(source).start()

    def settle(source):
        forwarded(source).wait_recv()
        landed(table, source, shsend, shrecv, source).wait_recv()

    def send_back(peer):
        pltpu.make_async_remote_copy(
            pbuf.at[peer], arrived.at[me], rssend.at[peer], rsrecv.at[me],
            device_id=(peer, t), device_id_type=MESH,
        ).start()

    rows = size * seqs
    pick = lax.broadcasted_iota(jnp.int32, (rows, lanes), 1) == me
    for k in range(parts):
        chunk = each(k, relay)
        if k == 0:
            for copy in local:
                copy.wait()
            for copy in remote:
                copy.wait()
        each(k, settle)
        span = pl.ds(chunk * size, size)
        low = g[0, span].reshape(rows, half)
        high = g[1, span].reshape(rows, half)

        def product(weight):
            return mm(low, weight[:half]) + mm(high, weight[half:])

        gate_logit = jnp.sum(low.astype(F32) * bgate_ref[:, :half], axis=1, keepdims=True) + jnp.sum(
            high.astype(F32) * bgate_ref[:, half:], axis=1, keepdims=True
        )
        gate_value = jax.nn.sigmoid(gate_logit)
        share = jnp.sum(
            jnp.where(pick, table[span].reshape(rows, lanes).astype(F32), 0.0),
            axis=1, keepdims=True,
        )
        expert_hidden = (jax.nn.silu(product(egb)) * product(eub)).astype(BF16)
        expert_row = mm(expert_hidden, edb[...]).astype(BF16).astype(F32)
        dense_hidden = (jax.nn.silu(product(dgb)) * product(dub)).astype(BF16)
        dense_sum = mm(dense_hidden, ddb[...])
        total = (share * expert_row + gate_value * dense_sum).astype(BF16)
        pbuf[span] = total.reshape(size, seqs, half)
        each(k, send_back)

    arrived[me] = pbuf[me]
    for k in range(parts):
        each(-k, lambda peer: landed(arrived, peer, rssend, rsrecv, peer).wait_recv())

    result = lax.fori_loop(
        0, n, lambda i, acc: acc + arrived[i].astype(F32), jnp.zeros((seqs, half), F32)
    )
    mid_half = jnp.where(t == 0, wide_mid[:, :half], wide_mid[:, half:])
    out_ref[...] = mid_half + result

    def drain(peer):
        to_peer(table, me, shsend, shrecv, peer).wait_send()
        to_peer(g, (t, me), agsend, agrecv, peer).wait_send()
        forward(peer).wait_send()
        pltpu.make_async_remote_copy(
            pbuf.at[peer], arrived.at[me], rssend.at[peer], rsrecv.at[me],
            device_id=(peer, t), device_id_type=MESH,
        ).wait_send()

    for k in range(parts):
        each(k, drain)


def trig_tables(cached):
    frequency = THETA ** (-np.arange(HD // 2, dtype=np.float32) * np.float32(2.0 / HD))
    frequency = np.tile(frequency.astype(np.float32).astype(np.float64), 4)
    rows = max(cached // TRIG_STEP + 1, TRIG_STEP)
    rows = -(-rows // 8) * 8
    high = (np.arange(rows) * TRIG_STEP)[:, None] * frequency[None]
    low = np.arange(rows)[:, None] * frequency[None]
    return np.stack([np.cos(high), np.sin(high), np.cos(low), np.sin(low)]).astype(np.float32)


def shards(
    tokens, mixer_gain, query_weight, key_weight, value_weight, head_lambda, head_gain,
    out_weight, cache_keys, cache_values, seq_lengths, channel_gain, expert_ids,
    expert_shares, expert_gate, expert_up, expert_down, dense_gate, dense_up, dense_down,
    branch_gate,
):
    n = lax.axis_size("ep")
    seqs, width = tokens.shape
    half = width // 2
    heads = head_lambda.shape[0]
    wide = 2 * HD
    block = 4 if seqs % 4 == 0 else 1
    lanes = -(-n // 128) * 128
    hidden = 2 * expert_gate.shape[2]
    units = dense_gate.shape[1]
    parts = 4 if n % 4 == 0 else 1
    vmem = pl.BlockSpec(memory_space=pltpu.VMEM)
    smem = pl.BlockSpec(memory_space=pltpu.SMEM)
    anyw = pl.BlockSpec(memory_space=pl.ANY)
    dma = pltpu.SemaphoreType.DMA
    trig = jnp.asarray(trig_tables(cache_keys.shape[1]))
    out = pl.pallas_call(
        functools.partial(layer_kernel, n, parts, block),
        out_shape=jax.ShapeDtypeStruct((seqs, half), F32),
        in_specs=[smem] * 2 + [vmem] * 8 + [anyw] * 12,
        out_specs=vmem,
        scratch_shapes=[
            pltpu.VMEM(query_weight.shape, BF16),
            pltpu.VMEM(key_weight.shape, BF16),
            pltpu.VMEM(value_weight.shape, BF16),
            pltpu.VMEM(out_weight.shape, BF16),
            pltpu.VMEM(cache_keys.shape, BF16),
            pltpu.VMEM(cache_values.shape, BF16),
            pltpu.VMEM((2, seqs, wide), F32),
            pltpu.VMEM((seqs, 2 * heads, wide), F32),
            pltpu.VMEM((seqs, wide), F32),
            pltpu.VMEM((seqs, wide), F32),
            pltpu.VMEM((heads, seqs, wide), F32),
            pltpu.VMEM((seqs, width), F32),
            pltpu.VMEM((2, n, seqs, half), BF16),
            pltpu.VMEM((n, seqs, lanes), BF16),
            pltpu.VMEM((seqs, width), F32),
            pltpu.VMEM((width, hidden), BF16),
            pltpu.VMEM((width, hidden), BF16),
            pltpu.VMEM((hidden, half), BF16),
            pltpu.VMEM((width, units), BF16),
            pltpu.VMEM((width, units), BF16),
            pltpu.VMEM((units, half), BF16),
            pltpu.VMEM((n, seqs, half), BF16),
            pltpu.VMEM((n, seqs, half), BF16),
            dma((4,)), dma((seqs // block,)), dma((seqs // block,)),
            dma((2,)), dma((6,)), dma((5,)), dma((5,)),
            dma((n,)), dma((n,)), dma((n,)), dma((n,)),
            dma((n,)), dma((n,)), dma((n,)), dma((n,)),
        ],
        compiler_params=pltpu.CompilerParams(collective_id=0, has_side_effects=True),
        name="layer",
    )(
        seq_lengths, head_lambda, expert_ids.T, expert_shares.T, tokens,
        mixer_gain.reshape(1, -1), head_gain.reshape(1, -1), channel_gain.reshape(1, -1),
        branch_gate.reshape(1, -1), trig, query_weight, key_weight, value_weight, out_weight,
        cache_keys, cache_values, expert_gate, expert_up, expert_down,
        dense_gate, dense_up, dense_down,
    )
    return out.astype(BF16)


def solution(mesh):
    placed = (
        P("ep", None), P(), P(None, "tp"), P(None, "tp"), P(None, "tp"), P("tp"), P(),
        P("tp", None), P("ep", None, "tp"), P("ep", None, "tp"), P("ep"), P(),
        P("ep", None), P("ep", None), P("ep", None, "tp"), P("ep", None, "tp"),
        P("ep", "tp", None), P("tp", "ep"), P("tp", "ep"), P("ep", "tp"), P(),
    )
    return jax.shard_map(
        shards, mesh=mesh, in_specs=placed, out_specs=P("ep", "tp"), check_vma=False
    )
```
